256 devices in a mesh: grp: 2 (over z), ep: 16 (over y, core), tp: 8 (over x).
Axes of the slice: x: 8, y: 8, z: 2, core: 2. Of those that a mesh axis runs over, the one named last changes fastest.
The devices are a block of a 8x8x16 slice.
Arguments:
- tokens: bfloat16 [12288, 4096], P(('grp', 'ep'), 'tp'), parts along dimension 0
- pre_gain: float32 [4096], replicated, may hold values from 0.1 to 1.9
- out_gain: float32 [4096], P('tp'), may hold values from 0.1 to 1.9
- chosen: int32 [32, 16, 48], P(('grp', 'ep')), parts along dimension 0, may hold values from 0 to 383, as said below
- route_weight: float32 [32, 16, 48], P(('grp', 'ep')), parts along dimension 0, may hold values from 0.3 to 3
- expert_gate: bfloat16 [16, 4096, 3072], P('ep', None, 'tp'), may hold values from -0.09375 to 0.09375
- expert_up: bfloat16 [16, 4096, 3072], P('ep', None, 'tp'), may hold values from -0.09375 to 0.09375
- expert_down: bfloat16 [16, 3072, 4096], P('ep', 'tp'), may hold values from -0.109375 to 0.109375
Outputs:
- output: bfloat16 [12288, 4096], P(('grp', 'ep'), 'tp'), parts along dimension 0
The draws below stay inside these ranges and needn't reach their ends.
There are 2 independent parts, one for each index of `grp`. The reference program is written for one: setup_inputs(seed, part) draws one part's arguments, and reference() takes and returns one part's arrays. A program takes and returns all parts, laid end to end along the dimension named above; an argument that names none is the same for every part. Nothing has to cross between parts.
Inputs may be any that keep to these rules, and one draw needn't show every extreme that they name: chosen[b, e, k] is the position, within block b of 384 tokens, of the k-th token that expert e takes from that block; the 48 positions of one block and one expert are all different.
All inputs are finite; a program needn't handle non-finite values.
Results may differ from the reference program's by a relative error of at most 0.0075.
Values may be sent and summed in bfloat16 or wider, within the bound.
A program may use at most 64 MiB of HBM per device.

```python
import math
import jax
import jax.numpy as jnp
from jax import lax

D = 4096
FF = 3072
TOK_DEV = 384
SLOT = 48
BLOCKS = 16
EXPERTS = 16
CAP = 768
TOKENS = 6144
N_TP = 8


def draw_tokens(key, part):
    key_base, key_rough, key_rows = jax.random.split(jax.random.fold_in(key, 11), 3)
    rough = jnp.exp(jax.random.uniform(key_rough, (D,), jnp.float32, -0.4, 0.4))
    row_scale = 0.5 * jnp.exp(jax.random.uniform(key_rows, (TOKENS, 1), jnp.float32, 0.0, math.log(10.0)))
    column_scale = jnp.exp(jnp.linspace(0.0, math.log(4.0), D, dtype=jnp.float32))
    base = jax.random.normal(key_base, (TOKENS, D), jnp.float32)
    return (base * column_scale * rough * row_scale).astype(jnp.bfloat16)


def draw_chosen(key, part):
    shape_all = (BLOCKS, EXPERTS, TOK_DEV)
    scores = jax.random.randint(jax.random.fold_in(key, 7), shape_all, 0, 1 << 20)
    scores = scores * TOK_DEV + lax.broadcasted_iota(jnp.int32, shape_all, 2)
    ranking = jnp.argsort(scores, axis=-1)
    return ranking[..., :SLOT].astype(jnp.int32)


def level_of(stream_key, dims, cuts, least, high):
    def one(axis_at, blocks):
        steps = jax.random.uniform(jax.random.fold_in(jax.random.fold_in(stream_key, 6), axis_at), (blocks,), jnp.float32, least / len(cuts), high / len(cuts))
        return jnp.repeat(jnp.exp(steps), dims[axis_at] // blocks).reshape((-1,) + (1,) * (len(dims) - axis_at - 1))

    level = one(*cuts[0])
    for cut in cuts[1:]:
        level = level * one(*cut)
    return level


def noise(key, extent, spread, limit, pieces=(), held_as=jnp.bfloat16):
    entries = jax.random.normal(key, extent, jnp.float32) * spread
    if len(pieces) > 0:
        entries = level_of(key, extent, pieces, -0.22, 0.18) * entries
    return jnp.clip(entries, min=-limit, max=limit).astype(held_as)


def setup_inputs(seed: int = 0, part: int = 0) -> dict:
    key_of = jax.random.split(jax.random.key(seed), 9)
    part_keys = jax.random.split(jax.random.fold_in(key_of[8], part), 9)
    tokens = draw_tokens(jax.random.fold_in(jax.random.fold_in(key_of[8], part), 71), part)
    pre_gain = jnp.clip(1.0 + 0.18 * jax.random.normal(key_of[1], (D,), jnp.float32), 0.1, 1.9)
    out_gain = jnp.clip(1.0 + 0.18 * jax.random.normal(key_of[2], (D,), jnp.float32), 0.1, 1.9)
    chosen = draw_chosen(jax.random.fold_in(jax.random.fold_in(key_of[8], part), 71), part)
    route_weight = jnp.clip(jnp.exp(math.log(3.0) - 2.3025851 * jax.random.uniform(part_keys[4], (BLOCKS, EXPERTS, SLOT), jnp.float32) ** level_of(part_keys[4], (BLOCKS, EXPERTS, SLOT), ((0, 16),), -0.2, 0.2)), 0.3, 3.0)
    expert_gate = noise(key_of[5], (EXPERTS, D, FF), D ** -0.5, 0.09375, ((0, 16), (2, 8)))
    expert_up = noise(key_of[6], (EXPERTS, D, FF), D ** -0.5, 0.09375, ((0, 16), (2, 8)))
    expert_down = noise(key_of[7], (EXPERTS, FF, D), FF ** -0.5, 0.109375, ((0, 16), (1, 8)))
    return dict(tokens=tokens, pre_gain=pre_gain, out_gain=out_gain, chosen=chosen, route_weight=route_weight, expert_gate=expert_gate, expert_up=expert_up, expert_down=expert_down)


NORM_EPS = 1e-06

def reference(tokens, pre_gain, out_gain, chosen, route_weight, expert_gate, expert_up, expert_down):
    resident = tokens.astype(jnp.float32)
    row_scale = lax.rsqrt(lax.optimization_barrier(jnp.mean(resident * resident, axis=1, keepdims=True)) + NORM_EPS)
    normed = (resident * row_scale * pre_gain).astype(jnp.bfloat16)
    offsets = (jnp.arange(BLOCKS, dtype=jnp.int32) * TOK_DEV)[:, None, None]
    global_index = jnp.transpose(chosen + offsets, (1, 0, 2)).reshape(EXPERTS, CAP).astype(jnp.int32)
    weights_flat = jnp.transpose(route_weight, (1, 0, 2)).reshape(EXPERTS, CAP)
    group_width = FF // N_TP

    def one_expert(operands):
        index_row, gate_matrix, up_matrix, down_matrix = operands
        picked_rows = jnp.take(normed, index_row, axis=0)
        gate_act = jnp.dot(picked_rows, gate_matrix, preferred_element_type=jnp.float32)
        up_act = jnp.dot(picked_rows, up_matrix, preferred_element_type=jnp.float32)
        hidden = (jax.nn.silu(gate_act) * up_act).astype(jnp.bfloat16)
        grouped = hidden.astype(jnp.float32).reshape(CAP, N_TP, group_width)
        down_groups = down_matrix.astype(jnp.float32).reshape(N_TP, group_width, D)
        partial_terms = jnp.einsum('cng,ngd->ncd', grouped, down_groups, precision=lax.Precision.HIGHEST).astype(jnp.bfloat16)
        partial_terms = lax.optimization_barrier(partial_terms)
        return lax.optimization_barrier(jnp.sum(partial_terms.astype(jnp.float32), axis=0)).astype(jnp.bfloat16)
    expert_out = lax.map(one_expert, (global_index, expert_gate, expert_up, expert_down))
    contributions = expert_out.astype(jnp.float32) * weights_flat[:, :, None]
    update = jnp.zeros((TOKENS, D), jnp.float32).at[global_index.reshape(-1)].add(contributions.reshape(-1, D))
    mixed_rows = resident + update
    out_scale = lax.rsqrt(lax.optimization_barrier(jnp.mean(mixed_rows * mixed_rows, axis=1, keepdims=True)) + NORM_EPS)
    return (mixed_rows * out_scale * out_gain).astype(jnp.bfloat16)
```

```python
import functools

import jax
import jax.numpy as jnp
from jax import lax
from jax.experimental import pallas as pl
from jax.experimental.pallas import tpu as pltpu
from jax.sharding import PartitionSpec as P

NORM_EPS = 1e-06
MESH = pl.DeviceIdType.MESH
RIGHT, LEFT = 0, 1
EVEN, ODD = 0, 1

SLOTS = {
    8: (7, {(RIGHT, EVEN): (0, 3, 6, 9), (RIGHT, ODD): (5, 8, 11),
            (LEFT, EVEN): (0, 3, 6), (LEFT, ODD): (2, 5, 8, 11)}),
    4: (3, {(RIGHT, EVEN): (0, 4), (RIGHT, ODD): (2,),
            (LEFT, EVEN): (0,), (LEFT, ODD): (1, 5)}),
}


def kernel(n_ep, n_tp, tokens, pre_gain, out_gain, chosen, route, w_gate, w_up, w_down,
           out,
           picks, gathered, normed, w_gu, w_dn, gate_up, hidden, partial, chain, summed,
           returned, mix_hi, mix_lo, mixed, squares,
           load_sem, disp_s, disp_r, ag_s, ag_r, rs_s, rs_r, ret_s, ret_r, sq_s, sq_r):
    bf16, f32 = jnp.bfloat16, jnp.float32
    tok, width = tokens.shape
    slots = chosen.shape[1]
    ffw = w_down.shape[0]
    chunk = 2 * slots
    n_y = n_ep // 2
    n_pair = n_y // 2
    rs0 = max(n_pair, 4)
    period, table = SLOTS[n_tp]
    model_width = n_tp * width

    ep = lax.axis_index("ep")
    tp = lax.axis_index("tp")
    y = ep // 2

    def wrap(v, n):
        return lax.rem(v + 2 * n, n)

    def rows(at, size):
        return pl.ds(pl.multiple_of(at * size, size), size)

    right, left = wrap(tp + 1, n_tp), wrap(tp - 1, n_tp)

    loads = [
        pltpu.make_async_copy(w_gate, w_gu.at[:, pl.ds(0, ffw)], load_sem.at[0]),
        pltpu.make_async_copy(w_up, w_gu.at[:, pl.ds(ffw, ffw)], load_sem.at[1]),
        pltpu.make_async_copy(w_down, w_dn, load_sem.at[2]),
    ]
    for load in loads:
        load.start()

    barrier = pltpu.get_barrier_semaphore()
    for k in range(1, n_ep):
        pl.semaphore_signal(barrier, inc=1, device_id={"ep": wrap(ep + k, n_ep)}, device_id_type=MESH)
    for k in range(1, n_tp):
        pl.semaphore_signal(barrier, inc=1, device_id={"tp": wrap(tp + k, n_tp)}, device_id_type=MESH)

    chosen_t = jnp.transpose(chosen[...].astype(f32))
    lane = lax.broadcasted_iota(jnp.int32, (slots, tok), 1).astype(f32)
    for e in range(n_ep):
        hot = jnp.where(chosen_t[:, e:e + 1] == lane, 1.0, 0.0).astype(bf16)
        picks[e * slots:(e + 1) * slots, :] = jnp.dot(
            hot, tokens[...], preferred_element_type=f32).astype(bf16)
    gathered[tp, rows(ep, slots), :] = picks[rows(ep, slots), :]

    pl.semaphore_wait(barrier, n_ep - 1 + n_tp - 1)

    def dispatch(e):
        return pltpu.make_async_remote_copy(
            src_ref=picks.at[rows(e, slots), :],
            dst_ref=gathered.at[tp, rows(ep, slots), :],
            send_sem=disp_s.at[e], recv_sem=disp_r.at[ep],
            device_id={"ep": e}, device_id_type=MESH)

    def dispatched(b):
        return pltpu.make_async_remote_copy(
            src_ref=picks.at[rows(b, slots), :],
            dst_ref=gathered.at[tp, rows(b, slots), :],
            send_sem=disp_s.at[b], recv_sem=disp_r.at[b],
            device_id={"ep": b}, device_id_type=MESH)

    dispatch(ep + 1 - 2 * lax.rem(ep, 2)).start()
    for j in range(n_pair):
        for rel in ((j, -j - 1) if j else (-1,)):
            for core in range(2):
                dispatch(2 * wrap(y + rel, n_y) + core).start()

    for row in range(0, tok, 128):
        mixed[row:row + 128, :] = tokens[row:row + 128, :].astype(f32)

    def chip_in(pair, par):
        return wrap(y - pair, n_y) if par == EVEN else wrap(y + pair + 1, n_y)

    def chip_back(step, par):
        pair = lax.rem(step + 1, n_pair)
        return wrap(y + pair + 1, n_y) if par == EVEN else wrap(y - pair, n_y)

    def ag(d, c, h):
        sign = 1 if d == RIGHT else -1
        at = (wrap(tp - sign * (h - 1), n_tp), rows(c, chunk), slice(None))
        return pltpu.make_async_remote_copy(
            src_ref=gathered.at[at], dst_ref=gathered.at[at],
            send_sem=ag_s.at[d, c, h - 1], recv_sem=ag_r.at[d, c, h - 1],
            device_id={"tp": right if d == RIGHT else left}, device_id_type=MESH)

    def ag_in(d, c, h):
        sign = 1 if d == RIGHT else -1
        at = (wrap(tp - sign * h, n_tp), rows(c, chunk), slice(None))
        return pltpu.make_async_remote_copy(
            src_ref=gathered.at[at], dst_ref=gathered.at[at],
            send_sem=ag_s.at[d, c, h - 1], recv_sem=ag_r.at[d, c, h - 1],
            device_id={"tp": left if d == RIGHT else right}, device_id_type=MESH)

    def rs(d, c, h, dest):
        src = partial.at[dest, rows(c, chunk), :] if h == 1 else chain.at[d, c, h - 2]
        return pltpu.make_async_remote_copy(
            src_ref=src, dst_ref=chain.at[d, c, h - 1],
            send_sem=rs_s.at[d, c, h - 1], recv_sem=rs_r.at[d, c, h - 1],
            device_id={"tp": right if d == RIGHT else left}, device_id_type=MESH)

    def wait_dispatched(c):
        for core in range(2):
            b = 2 * c + core

            @pl.when(b != ep)
            def _():
                dispatched(b).wait_recv()

    def send_gather(d, par, h, pair):
        c = chip_in(pair, par)
        if h > 1:
            ag_in(d, c, h - 1).wait_recv()
        ag(d, c, h).start()

    def send_reduce(d, par, h, step):
        hops = len(table[d, par])
        c = chip_back(step, par)
        sign = 1 if d == RIGHT else -1
        dest = wrap(tp + sign * (hops - h + 1), n_tp)
        if h > 1:
            rs(d, c, h - 1, dest).wait_recv()
            mine = partial[dest, rows(c, chunk), :].astype(f32)
            chain[d, c, h - 2] = (chain[d, c, h - 2].astype(f32) + mine).astype(bf16)
        rs(d, c, h, dest).start()

    def norm_pair(pair):
        for par in (EVEN, ODD):
            c = chip_in(pair, par)
            for d in (RIGHT, LEFT):
                ag_in(d, c, len(table[d, par])).wait_recv()
            total = jnp.zeros((chunk, 128), f32)
            for t in range(n_tp):
                for k in range(0, width, 128):
                    v = gathered[t, rows(c, chunk), k:k + 128].astype(f32)
                    total = total + v * v
            mean = jnp.sum(total, axis=1, keepdims=True) / model_width
            scale = lax.rsqrt(mean + NORM_EPS)
            for t in range(n_tp):
                v = gathered[t, rows(c, chunk), :].astype(f32)
                g = pre_gain[:, t * width:(t + 1) * width]
                normed[par * chunk:(par + 1) * chunk, t * width:(t + 1) * width] = (
                    v * scale * g).astype(bf16)

    gu_tile = 2 * ffw // 3 if (2 * ffw // 3) % 128 == 0 else 2 * ffw

    def gate_up_tile(n):
        at = slice(n * gu_tile, (n + 1) * gu_tile)
        gate_up[:, at] = jnp.dot(normed[...], w_gu[:, at], preferred_element_type=f32)

    def activate():
        g = gate_up[:, :ffw]
        u = gate_up[:, ffw:]
        hidden[...] = (g / (1.0 + jnp.exp(-g)) * u).astype(bf16)

    def down_tile(pair, t):
        res = jnp.dot(hidden[...], w_dn[:, t * width:(t + 1) * width],
                      preferred_element_type=f32).astype(bf16)
        partial[t, rows(chip_in(pair, EVEN), chunk), :] = res[:chunk]
        partial[t, rows(chip_in(pair, ODD), chunk), :] = res[chunk:]

    def mix_matrix(c):
        e = 2 * c
        picked = jnp.concatenate([chosen[pl.ds(e, 1), :], chosen[pl.ds(e + 1, 1), :]], axis=1)
        weight = jnp.concatenate([route[pl.ds(e, 1), :], route[pl.ds(e + 1, 1), :]], axis=1)
        for row in range(0, tok, 128):
            at = lax.broadcasted_iota(jnp.int32, (128, chunk), 0) + row
            w = jnp.where(at == picked, weight, 0.0)
            hi = w.astype(bf16)
            mix_hi[c, row:row + 128, :] = hi
            mix_lo[c, row:row + 128, :] = (w - hi.astype(f32)).astype(bf16)

    def give_back(e_block):
        return pltpu.make_async_remote_copy(
            src_ref=summed.at[rows(e_block, slots), :],
            dst_ref=returned.at[rows(ep, slots), :],
            send_sem=ret_s.at[e_block], recv_sem=ret_r.at[ep],
            device_id={"ep": e_block}, device_id_type=MESH)

    def given_back(e):
        return pltpu.make_async_remote_copy(
            src_ref=summed.at[rows(e, slots), :],
            dst_ref=returned.at[rows(e, slots), :],
            send_sem=ret_s.at[e], recv_sem=ret_r.at[e],
            device_id={"ep": e}, device_id_type=MESH)

    def finish_chunk(step, par):
        c = chip_back(step, par)
        total = partial[tp, rows(c, chunk), :].astype(f32)
        for d in (RIGHT, LEFT):
            hops = len(table[d, par])
            rs(d, c, hops, tp).wait_recv()
            total = total + chain[d, c, hops - 1].astype(f32)
        summed[rows(c, chunk), :] = total.astype(bf16)
        for core in range(2):
            b = 2 * c + core

            @pl.when(b != ep)
            def _():
                give_back(b).start()

            @pl.when(b == ep)
            def _():
                returned[rows(b, slots), :] = summed[rows(b, slots), :]

    def combine(step):
        pair = lax.rem(step + 1, n_pair)
        for c in (wrap(y - pair - 1, n_y), wrap(y + pair, n_y)):
            for core in range(2):
                e = 2 * c + core

                @pl.when(e != ep)
                def _():
                    given_back(e).wait_recv()
            rhs = returned[rows(c, chunk), :]
            mixed[...] += (jnp.dot(mix_hi[c], rhs, preferred_element_type=f32)
                           + jnp.dot(mix_lo[c], rhs, preferred_element_type=f32))

    n_gu = 2 * ffw // gu_tile
    pieces = [("norm",)] + [("gu", n) for n in range(n_gu)] + [("act",)] + [("dn", t) for t in range(n_tp)]
    share = -(-len(pieces) // (period - 1))

    def run_piece(piece, pair):
        if piece[0] == "norm":
            norm_pair(pair)
        elif piece[0] == "gu":
            gate_up_tile(piece[1])
        elif piece[0] == "act":
            activate()
        else:
            down_tile(pair, piece[1])

    last = rs0 + n_pair

    def round_(i, carry):
        @pl.when(i == 1)
        def _():
            for load in loads:
                load.wait()

        for k in range(period):
            for par, first in ((EVEN, 0), (ODD, min(table[RIGHT, ODD][0], table[LEFT, ODD][0]))):
                if first == k:
                    @pl.when(i < n_pair)
                    def _():
                        wait_dispatched(chip_in(i, par))
            for (d, par), offsets in table.items():
                for h, at in enumerate(offsets, 1):
                    if at % period != k:
                        continue
                    ii = i - at // period

                    @pl.when((ii >= 0) & (ii < n_pair))
                    def _():
                        send_gather(d, par, h, ii)

                    @pl.when((ii >= rs0) & (ii < rs0 + n_pair))
                    def _():
                        send_reduce(d, par, h, ii - rs0)

            pair = i - 2
            if k < period - 1:
                @pl.when((pair >= 0) & (pair < n_pair))
                def _():
                    for piece in pieces[k * share:(k + 1) * share]:
                        run_piece(piece, pair)

                if k == 0:
                    @pl.when(i < n_pair)
                    def _():
                        for par in (EVEN, ODD):
                            mix_matrix(chip_in(i, par))
        done = i - rs0 - 1

        @pl.when((done >= 0) & (done < n_pair))
        def _():
            for par in (EVEN, ODD):
                finish_chunk(done, par)

        @pl.when((done >= 1) & (done < n_pair))
        def _():
            combine(done - 1)
        return carry

    lax.fori_loop(0, last + 1, round_, 0)
    combine(n_pair - 1)

    part = jnp.zeros((tok, 128), f32)
    for k in range(0, width, 128):
        v = mixed[:, k:k + 128]
        part = part + v * v
    row_sum = lax.dot_general(jnp.ones((8, 128), f32), part, (((1,), (1,)), ((), ())),
                              precision=lax.Precision.HIGHEST, preferred_element_type=f32)
    squares[tp] = row_sum[0:1, :]

    def share_squares(peer):
        return pltpu.make_async_remote_copy(
            src_ref=squares.at[tp], dst_ref=squares.at[tp],
            send_sem=sq_s.at[peer], recv_sem=sq_r.at[tp],
            device_id={"tp": peer}, device_id_type=MESH)

    def shared_squares(peer):
        return pltpu.make_async_remote_copy(
            src_ref=squares.at[peer], dst_ref=squares.at[peer],
            send_sem=sq_s.at[peer], recv_sem=sq_r.at[peer],
            device_id={"tp": peer}, device_id_type=MESH)

    for k in range(1, n_tp):
        share_squares(wrap(tp + k, n_tp)).start()

    def sent_pair(pair, carry):
        for (d, par), offsets in table.items():
            for h in range(1, len(offsets) + 1):
                ag(d, chip_in(pair, par), h).wait_send()
                rs(d, chip_back(pair, par), h, tp).wait_send()
        return carry

    lax.fori_loop(0, n_pair, sent_pair, 0)

    def sent_block(k, carry):
        b = wrap(ep + k, n_ep)
        dispatch(b).wait_send()
        give_back(b).wait_send()
        return carry

    lax.fori_loop(1, n_ep, sent_block, 0)

    for k in range(1, n_tp):
        shared_squares(wrap(tp + k, n_tp)).wait_recv()
    total = squares[0]
    for t in range(1, n_tp):
        total = total + squares[t]
    scale_row = lax.rsqrt(total / model_width + NORM_EPS)
    scale = jnp.transpose(jnp.broadcast_to(scale_row, (8, tok)))[:, 0:1]
    out[...] = (mixed[...] * scale * out_gain[...]).astype(bf16)
    for k in range(1, n_tp):
        share_squares(wrap(tp + k, n_tp)).wait_send()


def solution(mesh):
    n_ep, n_tp = mesh.shape["ep"], mesh.shape["tp"]

    def shards(tokens, pre_gain, out_gain, chosen, route_weight, expert_gate, expert_up, expert_down):
        tok, width = tokens.shape
        slots = chosen.shape[2]
        ffw = expert_gate.shape[2]
        model_width = pre_gain.shape[0]
        cap = n_ep * slots
        chunk = 2 * slots
        n_y = n_ep // 2
        hops = n_tp // 2
        bf16, f32 = jnp.bfloat16, jnp.float32
        vmem = pl.BlockSpec(memory_space=pltpu.VMEM)
        hbm = pl.BlockSpec(memory_space=pl.ANY)
        dma = pltpu.SemaphoreType.DMA
        return pl.pallas_call(
            functools.partial(kernel, n_ep, n_tp),
            name="routed_ffn",
            out_shape=jax.ShapeDtypeStruct((tok, width), bf16),
            in_specs=[vmem] * 5 + [hbm] * 3,
            out_specs=vmem,
            scratch_shapes=[
                pltpu.VMEM((cap, width), bf16),
                pltpu.VMEM((n_tp, cap, width), bf16),
                pltpu.VMEM((2 * chunk, model_width), bf16),
                pltpu.VMEM((model_width, 2 * ffw), bf16),
                pltpu.VMEM((ffw, model_width), bf16),
                pltpu.VMEM((2 * chunk, 2 * ffw), f32),
                pltpu.VMEM((2 * chunk, ffw), bf16),
                pltpu.VMEM((n_tp, cap, width), bf16),
                pltpu.VMEM((2, n_y, hops, chunk, width), bf16),
                pltpu.VMEM((cap, width), bf16),
                pltpu.VMEM((cap, width), bf16),
                pltpu.VMEM((n_y, tok, chunk), bf16),
                pltpu.VMEM((n_y, tok, chunk), bf16),
                pltpu.VMEM((tok, width), f32),
                pltpu.VMEM((n_tp, 1, tok), f32),
                dma((3,)),
                dma((n_ep,)), dma((n_ep,)),
                dma((2, n_y, hops)), dma((2, n_y, hops)),
                dma((2, n_y, hops)), dma((2, n_y, hops)),
                dma((n_ep,)), dma((n_ep,)),
                dma((n_tp,)), dma((n_tp,)),
            ],
            compiler_params=pltpu.CompilerParams(
                collective_id=0, has_side_effects=True, vmem_limit_bytes=60 * 2**20),
        )(tokens, pre_gain.reshape(1, -1), out_gain.reshape(1, -1), chosen[0], route_weight[0],
          expert_gate[0], expert_up[0], expert_down[0])

    return jax.shard_map(
        shards,
        mesh=mesh,
        in_specs=(
            P(("grp", "ep"), "tp"),
            P(),
            P("tp"),
            P(("grp", "ep"), None, None),
            P(("grp", "ep"), None, None),
            P("ep", None, "tp"),
            P("ep", None, "tp"),
            P("ep", "tp", None),
        ),
        out_specs=P(("grp", "ep"), "tp"),
        check_vma=False,
    )
```

```python
import functools

import jax
import jax.numpy as jnp
from jax import lax
from jax.experimental import pallas as pl
from jax.experimental.pallas import tpu as pltpu
from jax.sharding import PartitionSpec as P

NORM_EPS = 1e-06
MESH = pl.DeviceIdType.MESH
RIGHT, LEFT = 0, 1
EVEN, ODD = 0, 1

SLOTS = {
    8: (7, {(RIGHT, EVEN): (0, 3, 6, 9), (RIGHT, ODD): (5, 8, 11),
            (LEFT, EVEN): (0, 3, 6), (LEFT, ODD): (2, 5, 8, 11)}),
    4: (3, {(RIGHT, EVEN): (0, 4), (RIGHT, ODD): (2,),
            (LEFT, EVEN): (0,), (LEFT, ODD): (1, 5)}),
}


def kernel(n_ep, n_tp, tokens_in, pre_gain_in, chosen_in, route_in, w_gate, w_up, w_down,
           mixed, scale_out,
           tokens, pre_gain, chosen, route, hot, picks, gathered, normed, w_gu, w_dn, gate_up, hidden,
           partial, chain, summed, returned, mix, squares,
           load_sem, disp_s, disp_r, ag_s, ag_r, rs_s, rs_r, ret_s, ret_r, sq_s, sq_r):
    bf16, f32 = jnp.bfloat16, jnp.float32
    tok, width = tokens.shape
    slots = chosen.shape[1]
    ffw = w_down.shape[0]
    chunk = 2 * slots
    n_y = n_ep // 2
    n_pair = n_y // 2
    rs0 = max(n_pair, 4)
    period, table = SLOTS[n_tp]
    model_width = n_tp * width

    ep = lax.axis_index("ep")
    tp = lax.axis_index("tp")
    y = ep // 2
    core = lax.rem(ep, 2)

    def wrap(v, n):
        return lax.rem(v + 2 * n, n)

    def rows(at, size):
        return pl.ds(pl.multiple_of(at * size, size), size)

    right, left = wrap(tp + 1, n_tp), wrap(tp - 1, n_tp)

    barrier = pltpu.get_barrier_semaphore()
    for k in range(1, n_ep):
        pl.semaphore_signal(barrier, inc=1, device_id={"ep": wrap(ep + k, n_ep)}, device_id_type=MESH)
    for k in range(1, n_tp):
        pl.semaphore_signal(barrier, inc=1, device_id={"tp": wrap(tp + k, n_tp)}, device_id_type=MESH)

    early = [pltpu.make_async_copy(src, dst, load_sem.at[k])
             for k, (src, dst) in enumerate(((chosen_in, chosen), (tokens_in, tokens)))]
    late = [pltpu.make_async_copy(src, dst, load_sem.at[k + 2])
            for k, (src, dst) in enumerate((
                (route_in, route), (pre_gain_in, pre_gain), (w_gate, w_gu.at[:, pl.ds(0, ffw)]),
                (w_up, w_gu.at[:, pl.ds(ffw, ffw)]), (w_down, w_dn)))]
    for load in early + late:
        load.start()

    early[0].wait()
    chosen_t = jnp.transpose(chosen[...].astype(f32))
    lane = lax.broadcasted_iota(jnp.int32, (slots, tok), 1).astype(f32)
    for e in range(n_ep):
        hot[e * slots:(e + 1) * slots, :] = jnp.where(chosen_t[:, e:e + 1] == lane, 1.0, 0.0).astype(bf16)
    early[1].wait()
    part_rows = n_ep * slots // 4
    for k in range(4):
        at = slice(k * part_rows, (k + 1) * part_rows)
        picks[at, :] = jnp.dot(hot[at, :], tokens[...], preferred_element_type=f32).astype(bf16)
    gathered[tp, rows(ep, slots), :] = picks[rows(ep, slots), :]

    pl.semaphore_wait(barrier, n_ep - 1 + n_tp - 1)

    def dispatch(e, to):
        return pltpu.make_async_remote_copy(
            src_ref=picks.at[rows(e, slots), :],
            dst_ref=gathered.at[tp, rows(to, slots), :],
            send_sem=disp_s.at[e], recv_sem=disp_r.at[to],
            device_id={"ep": e}, device_id_type=MESH)

    def chip_in(pair, par):
        return wrap(y - pair, n_y) if par == EVEN else wrap(y + pair + 1, n_y)

    def chip_back(step, par):
        pair = lax.rem(step + 1, n_pair)
        return wrap(y + pair + 1, n_y) if par == EVEN else wrap(y - pair, n_y)

    def blocks_in(c):
        return 2 * c + core, 2 * c + 1 - core

    def blocks_back(c):
        return 2 * c + 1 - core, 2 * c + core

    def ag(d, b, h, slice_at):
        sign = 1 if d == RIGHT else -1
        at = (wrap(tp - sign * slice_at, n_tp), rows(b, slots), slice(None))
        return pltpu.make_async_remote_copy(
            src_ref=gathered.at[at], dst_ref=gathered.at[at],
            send_sem=ag_s.at[d, b, h - 1], recv_sem=ag_r.at[d, b, h - 1],
            device_id={"tp": right if d == RIGHT else left}, device_id_type=MESH)

    def rs(d, b, h, dest):
        src = partial.at[dest, rows(b, slots), :] if h == 1 else chain.at[d, b, h - 2]
        return pltpu.make_async_remote_copy(
            src_ref=src, dst_ref=chain.at[d, b, h - 1],
            send_sem=rs_s.at[d, b, h - 1], recv_sem=rs_r.at[d, b, h - 1],
            device_id={"tp": right if d == RIGHT else left}, device_id_type=MESH)

    def wait_dispatched(b):
        @pl.when(b != ep)
        def _():
            dispatch(b, b).wait_recv()

    def gather_block(d, b, h):
        if h > 1:
            ag(d, b, h - 1, h - 1).wait_recv()
        ag(d, b, h, h - 1).start()

    def send_gather(d, par, h, pair):
        for b in blocks_in(chip_in(pair, par)):
            gather_block(d, b, h)

    def reduce_block(d, par, h, b):
        hops = len(table[d, par])
        sign = 1 if d == RIGHT else -1
        dest = wrap(tp + sign * (hops - h + 1), n_tp)
        if h > 1:
            rs(d, b, h - 1, dest).wait_recv()
            mine = partial[dest, rows(b, slots), :].astype(f32)
            chain[d, b, h - 2] = (chain[d, b, h - 2].astype(f32) + mine).astype(bf16)
        rs(d, b, h, dest).start()

    def send_reduce(d, par, h, step):
        for b in blocks_back(chip_back(step, par)):
            reduce_block(d, par, h, b)

    def norm_pair(pair):
        for par in (EVEN, ODD):
            c = chip_in(pair, par)
            for d in (RIGHT, LEFT):
                hops = len(table[d, par])
                for b in blocks_in(c):
                    ag(d, b, hops, hops).wait_recv()
            total = jnp.zeros((chunk, 128), f32)
            for t in range(n_tp):
                for k in range(0, width, 128):
                    v = gathered[t, rows(c, chunk), k:k + 128].astype(f32)
                    total = total + v * v
            mean = jnp.sum(total, axis=1, keepdims=True) / model_width
            scale = lax.rsqrt(mean + NORM_EPS)
            for t in range(n_tp):
                v = gathered[t, rows(c, chunk), :].astype(f32)
                g = pre_gain[:, t * width:(t + 1) * width]
                normed[par * chunk:(par + 1) * chunk, t * width:(t + 1) * width] = (
                    v * scale * g).astype(bf16)

    gu_tile = 2 * ffw // 3 if (2 * ffw // 3) % 128 == 0 else 2 * ffw

    def gate_up_tile(n):
        at = slice(n * gu_tile, (n + 1) * gu_tile)
        gate_up[:, at] = jnp.dot(normed[...], w_gu[:, at], preferred_element_type=f32)

    def activate():
        g = gate_up[:, :ffw]
        u = gate_up[:, ffw:]
        hidden[...] = (g / (1.0 + jnp.exp(-g)) * u).astype(bf16)

    def down_tile(pair, t):
        res = jnp.dot(hidden[...], w_dn[:, t * width:(t + 1) * width],
                      preferred_element_type=f32).astype(bf16)
        partial[t, rows(chip_in(pair, EVEN), chunk), :] = res[:chunk]
        partial[t, rows(chip_in(pair, ODD), chunk), :] = res[chunk:]

    def mix_matrix(c):
        e = 2 * c
        picked = jnp.concatenate([chosen[pl.ds(e, 1), :], chosen[pl.ds(e + 1, 1), :]], axis=1)
        weight = jnp.concatenate([route[pl.ds(e, 1), :], route[pl.ds(e + 1, 1), :]], axis=1)
        for row in range(0, tok, 128):
            at = lax.broadcasted_iota(jnp.int32, (128, chunk), 0) + row
            w = jnp.where(at == picked, weight, 0.0)
            hi = w.astype(bf16)
            lo = (w - hi.astype(f32)).astype(bf16)
            mix[c, row:row + 128, :] = jnp.concatenate([hi, lo], axis=1)

    def give_back(b, to):
        return pltpu.make_async_remote_copy(
            src_ref=summed.at[rows(b, slots), :],
            dst_ref=returned.at[rows(to, slots), :],
            send_sem=ret_s.at[b], recv_sem=ret_r.at[to],
            device_id={"ep": b}, device_id_type=MESH)

    def finish_block(par, b):
        total = partial[tp, rows(b, slots), :].astype(f32)
        for d in (RIGHT, LEFT):
            hops = len(table[d, par])
            rs(d, b, hops, tp).wait_recv()
            total = total + chain[d, b, hops - 1].astype(f32)
        total = total.astype(bf16)

        @pl.when(b != ep)
        def _():
            summed[rows(b, slots), :] = total
            give_back(b, ep).start()

        @pl.when(b == ep)
        def _():
            returned[rows(b, slots), :] = total

    def wait_returned(c):
        for k in range(2):
            e = 2 * c + k

            @pl.when(e != ep)
            def _():
                give_back(e, e).wait_recv()

    def chip_mixed(c, row):
        part = returned[rows(c, chunk), :]
        return mixed[row:row + 128, :] + jnp.dot(
            mix[c, row:row + 128, :], jnp.concatenate([part, part], axis=0), preferred_element_type=f32)

    def combine(c):
        wait_returned(c)
        for row in range(0, tok, 128):
            mixed[row:row + 128, :] = chip_mixed(c, row)

    def senders(step):
        pair = lax.rem(step + 1, n_pair)
        return wrap(y - pair - 1, n_y), wrap(y + pair, n_y)

    def gather_sent(pair):
        for (d, par), offsets in table.items():
            for b in blocks_in(chip_in(pair, par)):
                for h in range(1, len(offsets) + 1):
                    ag(d, b, h, h - 1).wait_send()

    def reduce_sent(step):
        for (d, par), offsets in table.items():
            for b in blocks_back(chip_back(step, par)):
                for h in range(1, len(offsets) + 1):
                    rs(d, b, h, tp).wait_send()

    n_gu = 2 * ffw // gu_tile
    pieces = [("norm",)] + [("gu", n) for n in range(n_gu)] + [("act",)] + [("dn", t) for t in range(n_tp)]
    share = -(-len(pieces) // (period - 1))

    def run_piece(piece, pair):
        if piece[0] == "norm":
            norm_pair(pair)
        elif piece[0] == "gu":
            gate_up_tile(piece[1])
        elif piece[0] == "act":
            activate()
        else:
            down_tile(pair, piece[1])

    own, twin = blocks_in(y)
    for d in (RIGHT, LEFT):
        gather_block(d, own, 1)
    dispatch(twin, ep).start()
    for j in range(n_pair):
        for rel in ((j, -j - 1) if j else (-1,)):
            for k in range(2):
                dispatch(2 * wrap(y + rel, n_y) + k, ep).start()
    wait_dispatched(twin)
    for d in (RIGHT, LEFT):
        gather_block(d, twin, 1)
    first = [(par, h, d) for (d, par), offsets in table.items()
             for h, at in enumerate(offsets, 1) if at < period]
    for par, h, d in sorted(m for m in first if m[0] == EVEN and m[1] > 1):
        send_gather(d, par, h, 0)
    for par, pair in ((ODD, 0), (EVEN, 1)):
        for b in blocks_in(chip_in(pair, par)):
            wait_dispatched(b)
            for d in (LEFT, RIGHT):
                gather_block(d, b, 1)
    for par, h, d in sorted(m for m in first if m[0] == ODD and m[1] > 1):
        send_gather(d, par, h, 0)
    for row in range(0, tok, 128):
        mixed[row:row + 128, :] = tokens[row:row + 128, :].astype(f32)

    last = rs0 + n_pair

    def round_(i, carry):
        for at, group in ((1, late[:1]), (2, late[1:])):
            @pl.when(i == at)
            def _():
                for load in group:
                    load.wait()

        for k in range(period):
            for par, at in ((EVEN, 0), (ODD, min(table[RIGHT, ODD][0], table[LEFT, ODD][0]))):
                if at == k:
                    @pl.when((i < n_pair) & (i != (1 if par == EVEN else 0)))
                    def _():
                        for b in blocks_in(chip_in(i, par)):
                            wait_dispatched(b)
            for (d, par), offsets in table.items():
                for h, at in enumerate(offsets, 1):
                    if at % period != k:
                        continue
                    ii = i - at // period

                    @pl.when((ii >= 0) & (ii < n_pair) & (ii != (1 if (par, h) == (EVEN, 1) else -1)))
                    def _():
                        send_gather(d, par, h, ii)

                    @pl.when((ii >= rs0) & (ii < rs0 + n_pair))
                    def _():
                        send_reduce(d, par, h, ii - rs0)

            pair = i - 2
            if k < period - 1:
                @pl.when((pair >= 0) & (pair < n_pair))
                def _():
                    for piece in pieces[k * share:(k + 1) * share]:
                        run_piece(piece, pair)

                if k == 0:
                    @pl.when(i <= n_pair)
                    def _():
                        for par in (EVEN, ODD):
                            mix_matrix(chip_in(i - 1, par))
                if k == 1:
                    @pl.when(i >= last - n_pair)
                    def _():
                        gather_sent(i - (last - n_pair))
        done = i - rs0 - 1

        @pl.when((done >= 0) & (done < n_pair))
        def _():
            for par in (EVEN, ODD):
                for b in blocks_back(chip_back(done, par)):
                    finish_block(par, b)

        @pl.when((done >= 1) & (done < n_pair))
        def _():
            for c in senders(done - 1):
                combine(c)
            reduce_sent(done - 1)
        return carry

    lax.fori_loop(1, last, round_, 0)

    end = n_pair - 1
    tail = sorted((at, d, par, h) for (d, par), offsets in table.items()
                  for h, at in enumerate(offsets, 1) if at >= period)
    cut = max(at for at, d, par, h in tail if par == EVEN)
    for at, d, par, h in tail:
        if at <= cut:
            send_reduce(d, par, h, end)
    combine(senders(end - 1)[0])
    for k in range(2):
        for at, d, par, h in tail:
            if at > cut:
                reduce_block(d, par, h, blocks_back(chip_back(end, par))[k])
    for b in blocks_back(chip_back(end, EVEN)):
        finish_block(EVEN, b)
    combine(senders(end - 1)[1])
    for b in blocks_back(chip_back(end, ODD)):
        finish_block(ODD, b)
    far, near = senders(end)
    combine(far)
    wait_returned(near)

    parts = []
    for row in range(0, tok, 128):
        v = chip_mixed(near, row)
        mixed[row:row + 128, :] = v
        v = v * v
        part = v[:, :128]
        for k in range(128, width, 128):
            part = part + v[:, k:k + 128]
        parts.append(part)
    row_sum = lax.dot_general(jnp.ones((8, 128), f32), jnp.concatenate(parts, axis=0),
                              (((1,), (1,)), ((), ())),
                              precision=lax.Precision.HIGHEST, preferred_element_type=f32)
    squares[tp] = row_sum[0:1, :]

    def share_squares(peer, at):
        return pltpu.make_async_remote_copy(
            src_ref=squares.at[at], dst_ref=squares.at[at],
            send_sem=sq_s.at[peer], recv_sem=sq_r.at[at],
            device_id={"tp": peer}, device_id_type=MESH)

    for k in range(n_tp // 2, 0, -1):
        for peer in {k, n_tp - k}:
            share_squares(wrap(tp + peer, n_tp), tp).start()

    reduce_sent(end - 1)
    reduce_sent(end)

    def sent_block(k, carry):
        b = wrap(ep + k, n_ep)
        dispatch(b, ep).wait_send()
        give_back(b, ep).wait_send()
        return carry

    lax.fori_loop(1, n_ep, sent_block, 0)

    for k in range(1, n_tp):
        peer = wrap(tp + k, n_tp)
        share_squares(peer, peer).wait_recv()
    total = squares[0]
    for t in range(1, n_tp):
        total = total + squares[t]
    scale_row = lax.rsqrt(total / model_width + NORM_EPS)
    scale = jnp.transpose(jnp.broadcast_to(scale_row, (8, tok)))[:, 0:1]
    scale_out[...] = jnp.broadcast_to(scale, scale_out.shape)
    for k in range(1, n_tp):
        share_squares(wrap(tp + k, n_tp), tp).wait_send()


def close(mixed, scale, out_gain, out):
    for k in range(0, out.shape[1], 128):
        out[:, k:k + 128] = (mixed[:, k:k + 128] * scale[...] * out_gain[:, k:k + 128]).astype(out.dtype)


def solution(mesh):
    n_ep, n_tp = mesh.shape["ep"], mesh.shape["tp"]

    def shards(tokens, pre_gain, out_gain, chosen, route_weight, expert_gate, expert_up, expert_down):
        tok, width = tokens.shape
        slots = chosen.shape[2]
        ffw = expert_gate.shape[2]
        model_width = pre_gain.shape[0]
        cap = n_ep * slots
        chunk = 2 * slots
        n_y = n_ep // 2
        hops = n_tp // 2
        bf16, f32 = jnp.bfloat16, jnp.float32
        vmem = pl.BlockSpec(memory_space=pltpu.VMEM)
        hbm = pl.BlockSpec(memory_space=pltpu.HBM)
        dma = pltpu.SemaphoreType.DMA
        mixed, scale = pl.pallas_call(
            functools.partial(kernel, n_ep, n_tp),
            name="routed_ffn",
            out_shape=(jax.ShapeDtypeStruct((tok, width), f32), jax.ShapeDtypeStruct((tok, 128), f32)),
            in_specs=[hbm] * 7,
            out_specs=(vmem, vmem),
            scratch_shapes=[
                pltpu.VMEM((tok, width), bf16),
                pltpu.VMEM((1, model_width), f32),
                pltpu.VMEM((n_ep, slots), jnp.int32),
                pltpu.VMEM((n_ep, slots), f32),
                pltpu.VMEM((cap, tok), bf16),
                pltpu.VMEM((cap, width), bf16),
                pltpu.VMEM((n_tp, cap, width), bf16),
                pltpu.VMEM((2 * chunk, model_width), bf16),
                pltpu.VMEM((model_width, 2 * ffw), bf16),
                pltpu.VMEM((ffw, model_width), bf16),
                pltpu.VMEM((2 * chunk, 2 * ffw), f32),
                pltpu.VMEM((2 * chunk, ffw), bf16),
                pltpu.VMEM((n_tp, cap, width), bf16),
                pltpu.VMEM((2, n_ep, hops, slots, width), bf16),
                pltpu.VMEM((cap, width), bf16),
                pltpu.VMEM((cap, width), bf16),
                pltpu.VMEM((n_y, tok, 2 * chunk), bf16),
                pltpu.VMEM((n_tp, 1, tok), f32),
                dma((7,)),
                dma((n_ep,)), dma((n_ep,)),
                dma((2, n_ep, hops)), dma((2, n_ep, hops)),
                dma((2, n_ep, hops)), dma((2, n_ep, hops)),
                dma((n_ep,)), dma((n_ep,)),
                dma((n_tp,)), dma((n_tp,)),
            ],
            compiler_params=pltpu.CompilerParams(
                collective_id=0, has_side_effects=True, vmem_limit_bytes=52 * 2**20),
        )(*(pltpu.with_memory_space_constraint(v, pltpu.HBM) for v in (
            tokens, pre_gain.reshape(1, -1), chosen[0], route_weight[0],
            expert_gate[0], expert_up[0], expert_down[0])))
        return pl.pallas_call(
            close,
            name="closing_norm",
            out_shape=jax.ShapeDtypeStruct((tok, width), bf16),
            in_specs=[vmem] * 3,
            out_specs=vmem,
            compiler_params=pltpu.CompilerParams(vmem_limit_bytes=8 * 2**20),
        )(mixed, scale, out_gain.reshape(1, -1))

    return jax.shard_map(
        shards,
        mesh=mesh,
        in_specs=(
            P(("grp", "ep"), "tp"),
            P(),
            P("tp"),
            P(("grp", "ep"), None, None),
            P(("grp", "ep"), None, None),
            P("ep", None, "tp"),
            P("ep", None, "tp"),
            P("ep", "tp", None),
        ),
        out_specs=P(("grp", "ep"), "tp"),
        check_vma=False,
    )
```

```python
import functools

import jax
import jax.numpy as jnp
from jax import lax
from jax.experimental import pallas as pl
from jax.experimental.pallas import tpu as pltpu
from jax.sharding import PartitionSpec as P

NORM_EPS = 1e-06
MESH = pl.DeviceIdType.MESH
RIGHT, LEFT = 0, 1
EVEN, ODD = 0, 1

SLOTS = {
    8: (7, {(RIGHT, EVEN): (0, 3, 6, 9), (RIGHT, ODD): (5, 8, 11),
            (LEFT, EVEN): (0, 3, 6), (LEFT, ODD): (2, 5, 8, 11)}),
    4: (3, {(RIGHT, EVEN): (0, 4), (RIGHT, ODD): (2,),
            (LEFT, EVEN): (0,), (LEFT, ODD): (1, 5)}),
}


def kernel(n_ep, n_tp, tokens_in, pre_gain_in, chosen_in, route_in, w_gate, w_up, w_down,
           mixed, scale_out,
           tokens, pre_gain, chosen, route, hot, picks, gathered, normed, w_gu, w_dn, gate_up, hidden,
           partial, chain, summed, returned, mix, squares,
           load_sem, disp_s, disp_r, ag_s, ag_r, rs_s, rs_r, ret_s, ret_r, sq_s, sq_r):
    bf16, f32 = jnp.bfloat16, jnp.float32
    tok, width = tokens.shape
    slots = chosen.shape[1]
    ffw = w_down.shape[0]
    chunk = 2 * slots
    n_y = n_ep // 2
    n_pair = n_y // 2
    rs0 = max(n_pair, 4)
    period, table = SLOTS[n_tp]
    model_width = n_tp * width

    ep = lax.axis_index("ep")
    tp = lax.axis_index("tp")
    y = ep // 2
    core = lax.rem(ep, 2)

    def wrap(v, n):
        return lax.rem(v + 2 * n, n)

    def rows(at, size):
        return pl.ds(pl.multiple_of(at * size, size), size)

    right, left = wrap(tp + 1, n_tp), wrap(tp - 1, n_tp)

    barrier = pltpu.get_barrier_semaphore()
    for k in range(1, n_ep):
        pl.semaphore_signal(barrier, inc=1, device_id={"ep": wrap(ep + k, n_ep)}, device_id_type=MESH)
    for k in range(1, n_tp):
        pl.semaphore_signal(barrier, inc=1, device_id={"tp": wrap(tp + k, n_tp)}, device_id_type=MESH)

    early = [pltpu.make_async_copy(src, dst, load_sem.at[k])
             for k, (src, dst) in enumerate(((chosen_in, chosen), (tokens_in, tokens)))]
    late = [pltpu.make_async_copy(src, dst, load_sem.at[k + 2])
            for k, (src, dst) in enumerate((
                (route_in, route), (pre_gain_in, pre_gain), (w_gate, w_gu.at[:, pl.ds(0, ffw)]),
                (w_up, w_gu.at[:, pl.ds(ffw, ffw)]), (w_down, w_dn)))]
    for load in early + late:
        load.start()

    early[0].wait()
    chosen_t = jnp.transpose(chosen[...].astype(f32))
    lane = lax.broadcasted_iota(jnp.int32, (slots, tok), 1).astype(f32)
    for e in range(n_ep):
        hot[e * slots:(e + 1) * slots, :] = jnp.where(chosen_t[:, e:e + 1] == lane, 1.0, 0.0).astype(bf16)
    early[1].wait()
    part_rows = n_ep * slots // 4
    for k in range(4):
        at = slice(k * part_rows, (k + 1) * part_rows)
        picks[at, :] = jnp.dot(hot[at, :], tokens[...], preferred_element_type=f32).astype(bf16)
    gathered[tp, rows(ep, slots), :] = picks[rows(ep, slots), :]

    pl.semaphore_wait(barrier, n_ep - 1 + n_tp - 1)

    def dispatch(e, to):
        return pltpu.make_async_remote_copy(
            src_ref=picks.at[rows(e, slots), :],
            dst_ref=gathered.at[tp, rows(to, slots), :],
            send_sem=disp_s.at[e], recv_sem=disp_r.at[to],
            device_id={"ep": e}, device_id_type=MESH)

    def chip_in(pair, par):
        return wrap(y - pair, n_y) if par == EVEN else wrap(y + pair + 1, n_y)

    def chip_back(step, par):
        pair = lax.rem(step + 1, n_pair)
        return wrap(y + pair + 1, n_y) if par == EVEN else wrap(y - pair, n_y)

    def blocks_in(c):
        return 2 * c + core, 2 * c + 1 - core

    def blocks_back(c):
        return 2 * c + 1 - core, 2 * c + core

    def ag(d, b, h, slice_at):
        sign = 1 if d == RIGHT else -1
        at = (wrap(tp - sign * slice_at, n_tp), rows(b, slots), slice(None))
        return pltpu.make_async_remote_copy(
            src_ref=gathered.at[at], dst_ref=gathered.at[at],
            send_sem=ag_s.at[d, b, h - 1], recv_sem=ag_r.at[d, b, h - 1],
            device_id={"tp": right if d == RIGHT else left}, device_id_type=MESH)

    def rs(d, b, h, dest):
        src = partial.at[dest, rows(b, slots), :] if h == 1 else chain.at[d, b, h - 2]
        return pltpu.make_async_remote_copy(
            src_ref=src, dst_ref=chain.at[d, b, h - 1],
            send_sem=rs_s.at[d, b, h - 1], recv_sem=rs_r.at[d, b, h - 1],
            device_id={"tp": right if d == RIGHT else left}, device_id_type=MESH)

    def wait_dispatched(b):
        @pl.when(b != ep)
        def _():
            dispatch(b, b).wait_recv()

    def gather_block(d, b, h):
        if h > 1:
            ag(d, b, h - 1, h - 1).wait_recv()
        ag(d, b, h, h - 1).start()

    def send_gather(d, par, h, pair):
        for b in blocks_in(chip_in(pair, par)):
            gather_block(d, b, h)

    def reduce_block(d, par, h, b):
        hops = len(table[d, par])
        sign = 1 if d == RIGHT else -1
        dest = wrap(tp + sign * (hops - h + 1), n_tp)
        if h > 1:
            rs(d, b, h - 1, dest).wait_recv()
            mine = partial[dest, rows(b, slots), :].astype(f32)
            chain[d, b, h - 2] = (chain[d, b, h - 2].astype(f32) + mine).astype(bf16)
        rs(d, b, h, dest).start()

    def send_reduce(d, par, h, step):
        for b in blocks_back(chip_back(step, par)):
            reduce_block(d, par, h, b)

    def norm_pair(pair):
        for par in (EVEN, ODD):
            c = chip_in(pair, par)
            for d in (RIGHT, LEFT):
                hops = len(table[d, par])
                for b in blocks_in(c):
                    ag(d, b, hops, hops).wait_recv()
            total = jnp.zeros((chunk, 128), f32)
            for t in range(n_tp):
                for k in range(0, width, 128):
                    v = gathered[t, rows(c, chunk), k:k + 128].astype(f32)
                    total = total + v * v
            mean = jnp.sum(total, axis=1, keepdims=True) / model_width
            scale = lax.rsqrt(mean + NORM_EPS)
            for t in range(n_tp):
                v = gathered[t, rows(c, chunk), :].astype(f32)
                g = pre_gain[:, t * width:(t + 1) * width]
                normed[par * chunk:(par + 1) * chunk, t * width:(t + 1) * width] = (
                    v * scale * g).astype(bf16)

    gu_tile = 2 * ffw // 3 if (2 * ffw // 3) % 128 == 0 else 2 * ffw

    def gate_up_tile(n):
        at = slice(n * gu_tile, (n + 1) * gu_tile)
        gate_up[:, at] = jnp.dot(normed[...], w_gu[:, at], preferred_element_type=f32)

    def activate():
        g = gate_up[:, :ffw]
        u = gate_up[:, ffw:]
        hidden[...] = (g / (1.0 + jnp.exp(-g)) * u).astype(bf16)

    def down_tile(pair, t):
        res = jnp.dot(hidden[...], w_dn[:, t * width:(t + 1) * width],
                      preferred_element_type=f32).astype(bf16)
        partial[t, rows(chip_in(pair, EVEN), chunk), :] = res[:chunk]
        partial[t, rows(chip_in(pair, ODD), chunk), :] = res[chunk:]

    def mix_matrix(c):
        e = 2 * c
        picked = jnp.concatenate([chosen[pl.ds(e, 1), :], chosen[pl.ds(e + 1, 1), :]], axis=1)
        weight = jnp.concatenate([route[pl.ds(e, 1), :], route[pl.ds(e + 1, 1), :]], axis=1)
        for row in range(0, tok, 128):
            at = lax.broadcasted_iota(jnp.int32, (128, chunk), 0) + row
            w = jnp.where(at == picked, weight, 0.0)
            hi = w.astype(bf16)
            lo = (w - hi.astype(f32)).astype(bf16)
            mix[c, row:row + 128, :] = jnp.concatenate([hi, lo], axis=1)

    def give_back(b, to):
        return pltpu.make_async_remote_copy(
            src_ref=summed.at[rows(b, slots), :],
            dst_ref=returned.at[rows(to, slots), :],
            send_sem=ret_s.at[b], recv_sem=ret_r.at[to],
            device_id={"ep": b}, device_id_type=MESH)

    def finish_block(par, b):
        total = partial[tp, rows(b, slots), :].astype(f32)
        for d in (RIGHT, LEFT):
            hops = len(table[d, par])
            rs(d, b, hops, tp).wait_recv()
            total = total + chain[d, b, hops - 1].astype(f32)
        total = total.astype(bf16)

        @pl.when(b != ep)
        def _():
            summed[rows(b, slots), :] = total
            give_back(b, ep).start()

        @pl.when(b == ep)
        def _():
            returned[rows(b, slots), :] = total

    def wait_returned(c):
        for k in range(2):
            e = 2 * c + k

            @pl.when(e != ep)
            def _():
                give_back(e, e).wait_recv()

    half = width // 2

    def chip_mixed(c, n):
        at = slice(n * half, (n + 1) * half)
        part = returned[rows(c, chunk), at]
        return mixed[:, at] + jnp.dot(
            mix[c], jnp.concatenate([part, part], axis=0), preferred_element_type=f32)

    def combine(c):
        wait_returned(c)
        for n in range(2):
            mixed[:, n * half:(n + 1) * half] = chip_mixed(c, n)

    def senders(step):
        pair = lax.rem(step + 1, n_pair)
        return wrap(y - pair - 1, n_y), wrap(y + pair, n_y)

    def gather_sent(pair):
        for (d, par), offsets in table.items():
            for b in blocks_in(chip_in(pair, par)):
                for h in range(1, len(offsets) + 1):
                    ag(d, b, h, h - 1).wait_send()

    def reduce_sent(step):
        for (d, par), offsets in table.items():
            for b in blocks_back(chip_back(step, par)):
                for h in range(1, len(offsets) + 1):
                    rs(d, b, h, tp).wait_send()

    n_gu = 2 * ffw // gu_tile
    pieces = [("norm",)] + [("gu", n) for n in range(n_gu)] + [("act",)] + [("dn", t) for t in range(n_tp)]
    share = -(-len(pieces) // (period - 1))

    def run_piece(piece, pair):
        if piece[0] == "norm":
            norm_pair(pair)
        elif piece[0] == "gu":
            gate_up_tile(piece[1])
        elif piece[0] == "act":
            activate()
        else:
            down_tile(pair, piece[1])

    own, twin = blocks_in(y)
    for d in (RIGHT, LEFT):
        gather_block(d, own, 1)
    dispatch(twin, ep).start()
    for j in range(n_pair):
        for rel in ((j, -j - 1) if j else (-1,)):
            for k in range(2):
                dispatch(2 * wrap(y + rel, n_y) + k, ep).start()
    wait_dispatched(twin)
    for d in (RIGHT, LEFT):
        gather_block(d, twin, 1)
    first = [(par, h, d) for (d, par), offsets in table.items()
             for h, at in enumerate(offsets, 1) if at < period]
    for par, h, d in sorted(m for m in first if m[0] == EVEN and m[1] > 1):
        send_gather(d, par, h, 0)
    for par, pair in ((ODD, 0), (EVEN, 1)):
        for b in blocks_in(chip_in(pair, par)):
            wait_dispatched(b)
            for d in (LEFT, RIGHT):
                gather_block(d, b, 1)
    for par, h, d in sorted(m for m in first if m[0] == ODD and m[1] > 1):
        send_gather(d, par, h, 0)
    for row in range(0, tok, 128):
        mixed[row:row + 128, :] = tokens[row:row + 128, :].astype(f32)

    last = rs0 + n_pair

    def round_(i, carry):
        for at, group in ((1, late[:1]), (2, late[1:])):
            @pl.when(i == at)
            def _():
                for load in group:
                    load.wait()

        for k in range(period):
            for par, at in ((EVEN, 0), (ODD, min(table[RIGHT, ODD][0], table[LEFT, ODD][0]))):
                if at == k:
                    @pl.when((i < n_pair) & (i != (1 if par == EVEN else 0)))
                    def _():
                        for b in blocks_in(chip_in(i, par)):
                            wait_dispatched(b)
            for (d, par), offsets in table.items():
                for h, at in enumerate(offsets, 1):
                    if at % period != k:
                        continue
                    ii = i - at // period

                    @pl.when((ii >= 0) & (ii < n_pair) & (ii != (1 if (par, h) == (EVEN, 1) else -1)))
                    def _():
                        send_gather(d, par, h, ii)

                    @pl.when((ii >= rs0) & (ii < rs0 + n_pair))
                    def _():
                        send_reduce(d, par, h, ii - rs0)

            pair = i - 2
            if k < period - 1:
                @pl.when((pair >= 0) & (pair < n_pair))
                def _():
                    for piece in pieces[k * share:(k + 1) * share]:
                        run_piece(piece, pair)

                if k == 0:
                    @pl.when(i <= n_pair)
                    def _():
                        for par in (EVEN, ODD):
                            mix_matrix(chip_in(i - 1, par))
                if k == 1:
                    @pl.when(i >= last - n_pair)
                    def _():
                        gather_sent(i - (last - n_pair))
                back = i - rs0 - 2
                for at, work in ((period - 3, lambda: combine(senders(back)[0])), (period - 2, lambda: combine(senders(back)[1])),
                                 (0, lambda: reduce_sent(back))):
                    if k == at:
                        @pl.when((back >= 0) & (back < n_pair))
                        def _():
                            work()
        done = i - rs0 - 1

        @pl.when((done >= 0) & (done < n_pair))
        def _():
            for par in (EVEN, ODD):
                for b in blocks_back(chip_back(done, par)):
                    finish_block(par, b)
        return carry

    lax.fori_loop(1, last, round_, 0)

    end = n_pair - 1
    tail = sorted((at, d, par, h) for (d, par), offsets in table.items()
                  for h, at in enumerate(offsets, 1) if at >= period)
    cut = max(at for at, d, par, h in tail if par == EVEN)
    for at, d, par, h in tail:
        if at <= cut:
            send_reduce(d, par, h, end)
    for k in range(2):
        for at, d, par, h in tail:
            if at > cut:
                reduce_block(d, par, h, blocks_back(chip_back(end, par))[k])
    reduce_sent(end - 1)
    for b in blocks_back(chip_back(end, EVEN)):
        finish_block(EVEN, b)
    for c in senders(end - 1):
        combine(c)
    for b in blocks_back(chip_back(end, ODD)):
        finish_block(ODD, b)
    far, near = senders(end)
    combine(far)
    wait_returned(near)

    part = jnp.zeros((tok, 128), f32)
    for n in range(2):
        v = chip_mixed(near, n)
        mixed[:, n * half:(n + 1) * half] = v
        for k in range(0, half, 128):
            w = v[:, k:k + 128]
            part = part + w * w
    squares[tp] = jnp.sum(jnp.transpose(part), axis=0, keepdims=True)

    def share_squares(peer, at):
        return pltpu.make_async_remote_copy(
            src_ref=squares.at[at], dst_ref=squares.at[at],
            send_sem=sq_s.at[peer], recv_sem=sq_r.at[at],
            device_id={"tp": peer}, device_id_type=MESH)

    for k in range(n_tp // 2, 0, -1):
        for peer in {k, n_tp - k}:
            share_squares(wrap(tp + peer, n_tp), tp).start()

    reduce_sent(end)

    def sent_block(k, carry):
        b = wrap(ep + k, n_ep)
        dispatch(b, ep).wait_send()
        give_back(b, ep).wait_send()
        return carry

    lax.fori_loop(1, n_ep, sent_block, 0)

    for k in range(1, n_tp):
        peer = wrap(tp + k, n_tp)
        share_squares(peer, peer).wait_recv()
    total = squares[0]
    for t in range(1, n_tp):
        total = total + squares[t]
    scale_row = lax.rsqrt(total / model_width + NORM_EPS)
    scale = jnp.transpose(jnp.broadcast_to(scale_row, (8, tok)))[:, 0:1]
    scale_out[...] = jnp.broadcast_to(scale, scale_out.shape)
    for k in range(1, n_tp):
        share_squares(wrap(tp + k, n_tp), tp).wait_send()


def close(mixed, scale, out_gain, out):
    for k in range(0, out.shape[1], 128):
        out[:, k:k + 128] = (mixed[:, k:k + 128] * scale[...] * out_gain[:, k:k + 128]).astype(out.dtype)


def solution(mesh):
    n_ep, n_tp = mesh.shape["ep"], mesh.shape["tp"]

    def shards(tokens, pre_gain, out_gain, chosen, route_weight, expert_gate, expert_up, expert_down):
        tok, width = tokens.shape
        slots = chosen.shape[2]
        ffw = expert_gate.shape[2]
        model_width = pre_gain.shape[0]
        cap = n_ep * slots
        chunk = 2 * slots
        n_y = n_ep // 2
        hops = n_tp // 2
        bf16, f32 = jnp.bfloat16, jnp.float32
        vmem = pl.BlockSpec(memory_space=pltpu.VMEM)
        hbm = pl.BlockSpec(memory_space=pltpu.HBM)
        dma = pltpu.SemaphoreType.DMA
        mixed, scale = pl.pallas_call(
            functools.partial(kernel, n_ep, n_tp),
            name="routed_ffn",
            out_shape=(jax.ShapeDtypeStruct((tok, width), f32), jax.ShapeDtypeStruct((tok, 128), f32)),
            in_specs=[hbm] * 7,
            out_specs=(vmem, vmem),
            scratch_shapes=[
                pltpu.VMEM((tok, width), bf16),
                pltpu.VMEM((1, model_width), f32),
                pltpu.VMEM((n_ep, slots), jnp.int32),
                pltpu.VMEM((n_ep, slots), f32),
                pltpu.VMEM((cap, tok), bf16),
                pltpu.VMEM((cap, width), bf16),
                pltpu.VMEM((n_tp, cap, width), bf16),
                pltpu.VMEM((2 * chunk, model_width), bf16),
                pltpu.VMEM((model_width, 2 * ffw), bf16),
                pltpu.VMEM((ffw, model_width), bf16),
                pltpu.VMEM((2 * chunk, 2 * ffw), f32),
                pltpu.VMEM((2 * chunk, ffw), bf16),
                pltpu.VMEM((n_tp, cap, width), bf16),
                pltpu.VMEM((2, n_ep, hops, slots, width), bf16),
                pltpu.VMEM((cap, width), bf16),
                pltpu.VMEM((cap, width), bf16),
                pltpu.VMEM((n_y, tok, 2 * chunk), bf16),
                pltpu.VMEM((n_tp, 1, tok), f32),
                dma((7,)),
                dma((n_ep,)), dma((n_ep,)),
                dma((2, n_ep, hops)), dma((2, n_ep, hops)),
                dma((2, n_ep, hops)), dma((2, n_ep, hops)),
                dma((n_ep,)), dma((n_ep,)),
                dma((n_tp,)), dma((n_tp,)),
            ],
            compiler_params=pltpu.CompilerParams(
                collective_id=0, has_side_effects=True, vmem_limit_bytes=52 * 2**20),
        )(*(pltpu.with_memory_space_constraint(v, pltpu.HBM) for v in (
            tokens, pre_gain.reshape(1, -1), chosen[0], route_weight[0],
            expert_gate[0], expert_up[0], expert_down[0])))
        return pl.pallas_call(
            close,
            name="closing_norm",
            out_shape=jax.ShapeDtypeStruct((tok, width), bf16),
            in_specs=[vmem] * 3,
            out_specs=vmem,
            compiler_params=pltpu.CompilerParams(vmem_limit_bytes=8 * 2**20),
        )(mixed, scale, out_gain.reshape(1, -1))

    return jax.shard_map(
        shards,
        mesh=mesh,
        in_specs=(
            P(("grp", "ep"), "tp"),
            P(),
            P("tp"),
            P(("grp", "ep"), None, None),
            P(("grp", "ep"), None, None),
            P("ep", None, "tp"),
            P("ep", None, "tp"),
            P("ep", "tp", None),
        ),
        out_specs=P(("grp", "ep"), "tp"),
        check_vma=False,
    )
```
